128 devices in a mesh: ep: 64 (over z, y, x), tp: 2 (over core).
Axes of the slice: x: 4, y: 4, z: 4, core: 2. Of those that a mesh axis runs over, the one named last changes fastest.
Arguments:
- tokens: bfloat16 [16384, 4096], P('ep'), may hold values from -6 to 6
- cotangent: bfloat16 [16384, 4096], P('ep'), may hold values from -1.5 to 1.5
- gates: float32 [16384, 2], P('ep'), may hold values from 0.05 to 0.95
- experts: int32 [16384, 2], P('ep'), may hold values from 0 to 63, all different within a row; in each aligned block of 256 rows (0 to 255, 256 to 511, ...) at most 12 rows name the same one
- gate_w: bfloat16 [64, 4096, 768], P('ep', None, 'tp'), may hold values from -0.09375 to 0.09375
- up_w: bfloat16 [64, 4096, 768], P('ep', None, 'tp'), may hold values from -0.09375 to 0.09375
- down_w: bfloat16 [64, 768, 4096], P('ep', 'tp'), may hold values from -0.21875 to 0.21875
Outputs:
- grad_tokens: bfloat16 [16384, 4096], P('ep', 'tp')
- grad_gates: float32 [16384, 2], P('ep')
- grad_gate_w: bfloat16 [64, 4096, 768], P('ep', None, 'tp')
- grad_up_w: bfloat16 [64, 4096, 768], P('ep', None, 'tp')
- grad_down_w: bfloat16 [64, 768, 4096], P('ep', 'tp')
- sq_gate: float32 [64, 4096], P('ep')
- sq_up: float32 [64, 4096], P('ep')
- sq_down: float32 [64, 768], P('ep', 'tp')
The draws below stay inside these ranges and needn't reach their ends.
Inputs may be any that keep to these rules, and one draw needn't show every extreme that they name: In each aligned block of 256 rows no expert is named by more than 12 rows, a bound that some expert reaches in some blocks; the 2 experts of a row differ.
All inputs are finite; a program needn't handle non-finite values.
Results may differ from the reference program's by a relative error of at most 0.024.
Values may be sent and summed in bfloat16 or wider, within the bound.
A program may use at most 192 MiB of HBM per device.

```python
import math
import jax
import jax.numpy as jnp
import numpy as np
from jax import lax

D = 4096
FF = 768
TOPK = 2
TOK_DEV = 256
EXPERTS = 64
CAP = 12
TOKENS = 16384
N_EP = 64
N_TP = 2


def level_of(key, dims, shards, low, top_value):
    factor_of, own = 1.0, jax.random.fold_in(key, 6)
    for position, shards_of in shards:
        heights = jnp.exp(jax.random.uniform(jax.random.fold_in(own, position), (shards_of,), jnp.float32, low / len(shards), top_value / len(shards)))
        factor_of = factor_of * jnp.repeat(heights, dims[position] // shards_of).reshape([-1 if axis == position else 1 for axis in range(len(dims))])
    return factor_of


def shared_out(own_key, own, number, rows, number_of, top, bound, lean):
    sequence = jax.random.permutation(own_key, number_of)
    crowded, ordinary = load_shares(number_of, rows * top, bound, lean, True), load_shares(number_of, rows * top, bound, lean, False)
    places = jnp.arange(number_of)

    def named(sizes, offset_by):
        used = int((sizes > 0).sum())
        fixed = max(1, used // 4)
        moved = fixed + (places - fixed + offset_by * (used - fixed)) % max(1, number_of - fixed)
        return jnp.zeros((number_of,), jnp.int32).at[sequence[jnp.where(places < fixed, places, moved)]].set(jnp.asarray(sizes, jnp.int32))

    sizes = jnp.where(number % 4 == 0, named(crowded, number // 4), named(ordinary, number - number // 4 - 1))
    mixed = jax.random.permutation(jax.random.fold_in(own, 3), number_of)
    source_of, sink = mixed[0:number_of // 2 * 2:2], mixed[1:number_of // 2 * 2:2]
    slack = jnp.minimum(sizes[source_of] - 1, bound - sizes[sink]) // 2
    slack = jnp.where((source_of == sequence[0]) | (sink == sequence[0]) | (sizes[sink] == 0), 0, jnp.maximum(slack, 0))
    moved = jax.random.randint(jax.random.fold_in(own, 4), (number_of // 2,), 0, 1 << 20) % (slack + 1)
    sizes = sizes.at[source_of].add(-moved).at[sink].add(moved)
    items = jnp.searchsorted(jnp.cumsum(sizes), jnp.arange(rows * top), side="right").astype(jnp.int32)
    grid = items.reshape(top, rows).T
    grid = grid[jax.random.permutation(jax.random.fold_in(own, 1), rows)]
    offset_by = jax.random.randint(jax.random.fold_in(own, 2), (rows, 1), 0, top)
    return jnp.take_along_axis(grid, (jnp.arange(top)[None, :] + offset_by) % top, axis=1)


def load_shares(number_of, total, limit, lean, full):
    weights = [(1 << 20) // math.isqrt(grade ** lean) + 1 for grade in range(1, number_of + 1)]
    largest = limit if full else min(limit, max(-(-total // number_of), total * weights[0] // sum(weights)))
    least = 1 if total - largest >= number_of - 1 else 0
    given, rest = [largest] + [least] * (number_of - 1), total - largest - least * (number_of - 1)
    while rest > 0:
        movable = [i for i in range(1, number_of) if given[i] < largest] or [i for i in range(1, number_of) if given[i] < limit]
        whole, budget = sum([weights[i] for i in movable]), rest
        for i in movable:
            addition = min(limit - given[i], max(1, budget * weights[i] // whole), rest)
            given[i] = given[i] + addition
            rest = rest - addition
    return np.array(given)


def bell_draw(key, extent, width, most, split=(), kind=jnp.bfloat16):
    array = jax.random.normal(key, extent, jnp.float32) * width
    if len(split) > 0:
        array = level_of(key, extent, split, -0.22, 0.18) * array
    return jnp.clip(array, min=-most, max=most).astype(kind)


def setup_inputs(seed: int = 0) -> dict:
    streams_of = jax.random.split(jax.random.key(seed), 8)
    tokens = bell_draw(streams_of[0], (TOKENS, D), 1.0, 6.0, ((0, 64),))
    cotangent = bell_draw(streams_of[1], (TOKENS, D), 0.25, 1.5, ((0, 64),))
    gates = jnp.clip(0.05 + 0.9 * jax.random.uniform(streams_of[2], (TOKENS, TOPK), jnp.float32) ** level_of(streams_of[2], (TOKENS, TOPK), ((0, 64),), -0.2, 0.2), 0.05, 0.95)
    experts_keys = jax.random.split(jax.random.fold_in(streams_of[3], 1), TOKENS // TOK_DEV)
    experts_turns = jax.random.permutation(jax.random.fold_in(streams_of[3], 3), TOKENS // TOK_DEV)
    experts = jax.vmap(lambda own, number: shared_out(jax.random.fold_in(streams_of[3], 2), own, number, TOK_DEV, EXPERTS, TOPK, CAP, 2))(experts_keys, experts_turns).reshape((TOKENS, TOPK))
    gate_w = bell_draw(streams_of[4], (EXPERTS, D, FF), D ** -0.5, 0.09375, ((0, 64), (2, 2)))
    up_w = bell_draw(streams_of[5], (EXPERTS, D, FF), D ** -0.5, 0.09375, ((0, 64), (2, 2)))
    down_w = bell_draw(streams_of[6], (EXPERTS, FF, D), FF ** -0.5, 0.21875, ((0, 64), (1, 2)))
    return dict(tokens=tokens, cotangent=cotangent, gates=gates, experts=experts, gate_w=gate_w, up_w=up_w, down_w=down_w)


def expert_terms(w_gate, w_up, w_down, indices, tokens, cotangent, gates):
    n_assign = TOKENS * TOPK
    valid = indices < n_assign
    safe = jnp.minimum(indices, n_assign - 1)
    tok_index = safe // TOPK
    rows_x = jnp.where(valid[:, None], tokens[tok_index], jnp.zeros((), jnp.bfloat16)).astype(jnp.bfloat16)
    rows_dy = jnp.where(valid[:, None], cotangent[tok_index], jnp.zeros((), jnp.bfloat16)).astype(jnp.bfloat16)
    rows_g = jnp.where(valid, gates.reshape(-1)[safe], jnp.zeros((), jnp.float32))
    pre_gate = jnp.dot(rows_x, w_gate, preferred_element_type=jnp.float32)
    pre_up = jnp.dot(rows_x, w_up, preferred_element_type=jnp.float32)
    sigmoid_gate = jax.nn.sigmoid(pre_gate)
    silu_gate = pre_gate * sigmoid_gate
    hidden = (silu_gate * pre_up).astype(jnp.bfloat16)
    hidden_grad = jnp.dot(rows_dy, w_down.T, preferred_element_type=jnp.float32)
    gate_sum = jnp.sum(hidden.astype(jnp.float32) * hidden_grad, axis=1)
    scaled = rows_g[:, None] * hidden_grad
    grad_pre_gate = (scaled * pre_up * sigmoid_gate * (1.0 + pre_gate * (1.0 - sigmoid_gate))).astype(jnp.bfloat16)
    grad_pre_up = (scaled * silu_gate).astype(jnp.bfloat16)
    weighted = (rows_g[:, None] * hidden.astype(jnp.float32)).astype(jnp.bfloat16)
    grad_dw = jnp.dot(weighted.T, rows_dy, preferred_element_type=jnp.float32).astype(jnp.bfloat16)
    grad_gw = jnp.dot(rows_x.T, grad_pre_gate, preferred_element_type=jnp.float32).astype(jnp.bfloat16)
    grad_uw = jnp.dot(rows_x.T, grad_pre_up, preferred_element_type=jnp.float32).astype(jnp.bfloat16)
    rows = rows_x.shape[0]
    block_units = FF // N_TP
    split_gate = grad_pre_gate.astype(jnp.float32).reshape(rows, N_TP, block_units)
    split_up = grad_pre_up.astype(jnp.float32).reshape(rows, N_TP, block_units)
    wg_split = w_gate.astype(jnp.float32).reshape(D, N_TP, block_units)
    wu_split = w_up.astype(jnp.float32).reshape(D, N_TP, block_units)
    partial_value = jnp.einsum('rhf,dhf->rhd', split_gate, wg_split) + jnp.einsum('rhf,dhf->rhd', split_up, wu_split)
    partial_value = partial_value.astype(jnp.bfloat16).astype(jnp.float32)
    row_grad = jnp.sum(partial_value, axis=1).astype(jnp.bfloat16)
    return grad_gw, grad_uw, grad_dw, row_grad, gate_sum


def reference(tokens, cotangent, gates, experts, gate_w, up_w, down_w):
    n_assign = TOKENS * TOPK
    flat_ids = experts.reshape(N_EP, TOK_DEV * TOPK)
    onehot = (flat_ids[:, :, None] == jnp.arange(EXPERTS, dtype=jnp.int32)[None, None, :]).astype(jnp.int32)
    earlier = jnp.cumsum(onehot, axis=1) - onehot
    slot_of = jnp.sum(earlier * onehot, axis=2).astype(jnp.int32)
    block_id = jnp.broadcast_to(jnp.arange(N_EP, dtype=jnp.int32)[:, None], flat_ids.shape)
    numbers = jnp.arange(n_assign, dtype=jnp.int32).reshape(N_EP, TOK_DEV * TOPK)
    table = jnp.full((EXPERTS, N_EP, CAP), n_assign, jnp.int32).at[flat_ids, block_id, slot_of].set(numbers)
    table = table.reshape(EXPERTS, N_EP * CAP)

    def per_expert(args):
        w_gate, w_up, w_down, indices = args
        return expert_terms(w_gate, w_up, w_down, indices, tokens, cotangent, gates)

    grad_gw, grad_uw, grad_dw, row_grad, gate_sum = lax.map(per_expert, (gate_w, up_w, down_w, table))
    flat_index = table.reshape(-1)
    tok_target = jnp.where(flat_index < n_assign, flat_index // TOPK, TOKENS).astype(jnp.int32)
    grad_tokens = jnp.zeros((TOKENS, D), jnp.float32).at[tok_target].add(
        row_grad.reshape(-1, D).astype(jnp.float32), mode="drop").astype(jnp.bfloat16)
    grad_gates = jnp.zeros((n_assign,), jnp.float32).at[flat_index].set(
        gate_sum.reshape(-1), mode="drop").reshape(TOKENS, TOPK)
    gw_f = grad_gw.astype(jnp.float32)
    uw_f = grad_uw.astype(jnp.float32)
    dw_f = grad_dw.astype(jnp.float32)
    sq_gate = jnp.sum(gw_f * gw_f, axis=2) / FF
    sq_up = jnp.sum(uw_f * uw_f, axis=2) / FF
    sq_down = jnp.sum(dw_f * dw_f, axis=2) / D
    return (grad_tokens, grad_gates, grad_gw, grad_uw, grad_dw, sq_gate, sq_up, sq_down)
```

```python
import functools

import jax
import jax.numpy as jnp
from jax import lax
from jax.experimental import pallas as pl
from jax.experimental.pallas import tpu as pltpu
from jax.sharding import PartitionSpec as P

MESH = pl.DeviceIdType.MESH
F32 = jnp.float32
BF16 = jnp.bfloat16
I32 = jnp.int32
CAP = 12
SIDE = 4
CH = 512
NT = (((1,), (1,)), ((), ()))
TN = (((0,), (0,)), ((), ()))
HI = lax.Precision.HIGHEST


def mm(a, b):
    return jnp.dot(a, b, preferred_element_type=F32)


def iota(shape, dim):
    return lax.broadcasted_iota(I32, shape, dim)


def hot(mask):
    return jnp.where(mask, 1.0, 0.0).astype(BF16)


def offsets(p, div, rem):
    q = div(p, 16)
    a = rem(div(p, 8), 2)
    d = rem(div(p, 4), 2)
    oy = rem(p, 4)
    ox = rem(oy + 2 * a + d, 4)
    oz = rem(q + 8 - oy - ox, 4)
    return oz, oy, ox


def scalar_div(a, b):
    return lax.div(a, jnp.int32(b))


def scalar_rem(a, b):
    return lax.rem(a, jnp.int32(b))


def vector_div(a, b):
    return a >> (b.bit_length() - 1)


def vector_rem(a, b):
    return a & (b - 1)


def kernel(
    gs,
    exp_c, exp_r, gat_r, tok, cot, gw, uw, dw,
    gt_o, gg_o, ggw_o, guw_o, gdw_o, sqg_o, squ_o, sqd_o,
    tokv, wgu, wd, send, recv, xv, yv, gp, wt, psend, own, precv, back, gtv, pm, qm,
    gsend, grecv, gps, gpr, rgs, bg, sqs, sqr, sqa,
    d_s, d_r, dg_s, dg_r, f_s, f_r, p_s, p_r, pg_s, pg_r, r_s, r_r, rg_s, rg_r, sq_s, sq_r, ld, st,
):
    n_pos = SIDE ** 3
    ng = n_pos // gs
    wr = 16 * gs
    cr = CAP * gs
    rows_tok, half = tokv.shape[1], tokv.shape[2]
    width = 2 * half
    fold = half - CH
    nk = fold // CH
    ff = wd.shape[0]
    ep = lax.axis_index("ep")
    core = lax.axis_index("tp")
    other = 1 - core
    cz = scalar_div(ep, 16)
    cy = scalar_rem(scalar_div(ep, 4), 4)
    cx = scalar_rem(ep, 4)

    def dest_of(p):
        oz, oy, ox = offsets(p, scalar_div, scalar_rem)
        return (
            scalar_rem(cz + oz, 4) * 16 + scalar_rem(cy + oy, 4) * 4 + scalar_rem(cx + ox, 4)
        )

    def source_of(p):
        oz, oy, ox = offsets(p, scalar_div, scalar_rem)
        return (
            scalar_rem(cz + 4 - oz, 4) * 16
            + scalar_rem(cy + 4 - oy, 4) * 4
            + scalar_rem(cx + 4 - ox, 4)
        )

    def expert_vec(p):
        oz, oy, ox = offsets(p, vector_div, vector_rem)
        return ((cz + oz) & 3) * 16 + ((cy + oy) & 3) * 4 + ((cx + ox) & 3)

    def remote(src, dst, ssem, rsem, ids):
        return pltpu.make_async_remote_copy(
            src_ref=src, dst_ref=dst, send_sem=ssem, recv_sem=rsem,
            device_id=ids, device_id_type=MESH,
        )

    barrier = pltpu.get_barrier_semaphore()

    def greet(p, carry):
        pl.semaphore_signal(
            barrier, inc=1, device_id={"ep": dest_of(p)}, device_id_type=MESH
        )
        return carry

    lax.fori_loop(1, n_pos, greet, 0)
    pl.semaphore_signal(barrier, inc=1, device_id={"tp": other}, device_id_type=MESH)
    mine = pl.ds(pl.multiple_of(core * half, half), half)
    loads = [
        pltpu.make_async_copy(tok.at[:, mine], tokv.at[0], ld.at[0]),
        pltpu.make_async_copy(cot.at[:, mine], tokv.at[1], ld.at[1]),
        pltpu.make_async_copy(gw, wgu.at[:, 0:ff], ld.at[2]),
        pltpu.make_async_copy(uw, wgu.at[:, ff : 2 * ff], ld.at[3]),
        pltpu.make_async_copy(dw, wd, ld.at[4]),
    ]
    for copy in loads:
        copy.start()

    e_lane = [exp_r[j : j + 1, :] for j in range(2)]
    e_sub = [exp_c[:, j : j + 1] for j in range(2)]
    hot_t = [
        jnp.where(iota((n_pos, rows_tok), 0) == e_lane[j], 1.0, 0.0).astype(F32) for j in range(2)
    ]
    hot_c = [
        jnp.where(iota((rows_tok, n_pos), 1) == e_sub[j], 1.0, 0.0).astype(F32) for j in range(2)
    ]
    upper = hot(iota((rows_tok, rows_tok), 0) < iota((rows_tok, rows_tok), 1))
    lower = hot(iota((rows_tok, rows_tok), 1) < iota((rows_tok, rows_tok), 0))
    prior_t = mm((hot_t[0] + hot_t[1]).astype(BF16), upper)
    prior_c = mm(lower, (hot_c[0] + hot_c[1]).astype(BF16))
    slot_lane = [
        jnp.sum(hot_t[j] * prior_t, axis=0, keepdims=True).astype(I32) for j in range(2)
    ]
    slot_sub = [
        jnp.sum(hot_c[j] * prior_c, axis=1, keepdims=True).astype(I32) for j in range(2)
    ]
    key_lane = [e_lane[j] * 16 + slot_lane[j] for j in range(2)]
    key_sub = [e_sub[j] * 16 + slot_sub[j] for j in range(2)]

    place = expert_vec(iota((n_pos, rows_tok), 0))
    gate_rows = jnp.zeros((n_pos, 128), F32)
    for j in range(2):
        picked = jnp.where(place == e_lane[j], gat_r[j : j + 1, :], 0.0)
        slots = jnp.where(iota((rows_tok, 128), 1) == slot_sub[j], 1.0, 0.0)
        gate_rows += jnp.dot(picked, slots, preferred_element_type=F32, precision=HI)
    gsend[...] = gate_rows.reshape(n_pos, 1, 128)

    to_c, of_w = iota((cr, wr), 0), iota((cr, wr), 1)
    wire_r, wire_s = of_w & 15, of_w >> 4
    pm[0] = hot((wire_r < CAP) & (to_c == CAP * wire_s + wire_r))
    for k in range(nk):
        pm[1 + k] = hot((wire_r >= CAP) & (to_c == CAP * wire_s + 4 * k + wire_r - CAP))
    of_w, to_c = iota((wr, cr), 0), iota((wr, cr), 1)
    wire_r, wire_s = of_w & 15, of_w >> 4
    qm[0] = hot((wire_r < CAP) & (to_c == CAP * wire_s + wire_r))
    for k in range(nk):
        qm[1 + k] = hot((wire_r >= CAP) & (to_c == CAP * wire_s + 4 * k + wire_r - CAP))

    loads[0].wait()
    loads[1].wait()

    def wire_rows(g):
        return pl.ds(pl.multiple_of(g * wr, wr), wr)

    def block_rows(p):
        return pl.ds(pl.multiple_of(p * 16, 16), 16)

    def dispatch(g, carry):
        row = iota((wr, rows_tok), 0)
        r = row & 15
        base = expert_vec(g * gs + (row >> 4)) * 16
        direct = base + r
        folded = jnp.where(r >= CAP, base + r - CAP, -4096)
        s_dir = hot((key_lane[0] == direct) | (key_lane[1] == direct))
        s_fold = [
            hot((key_lane[0] == folded + 4 * k) | (key_lane[1] == folded + 4 * k))
            for k in range(nk)
        ]
        for a in range(2):
            last = tokv[a, :, fold : fold + CH]
            for k in range(nk):
                part = mm(s_dir, tokv[a, :, k * CH : (k + 1) * CH]) + mm(s_fold[k], last)
                send[wire_rows(g), a * fold + k * CH : a * fold + (k + 1) * CH] = part.astype(BF16)

        @pl.when(g == 0)
        def _():
            pl.semaphore_wait(barrier, n_pos)
            recv[core, 0:16, :] = send[0:16, :]
            grecv[0] = gsend[0]

        def start(i, carry):
            p = g * gs + i

            @pl.when(p > 0)
            def _():
                dest = {"ep": dest_of(p)}
                remote(
                    gsend.at[p], grecv.at[p], dg_s.at[g], dg_r.at[g], dest
                ).start()
                remote(
                    send.at[block_rows(p)], recv.at[core, block_rows(p)],
                    d_s.at[g], d_r.at[g], dest,
                ).start()

            return carry

        lax.fori_loop(0, gs, start, 0)
        return carry

    lax.fori_loop(0, ng, dispatch, 0)
    for copy in loads[2:]:
        copy.wait()

    def group_wait(g, make, recv_side):
        @pl.when(g == 0)
        def _():
            copy = make(1, gs - 1)
            copy.wait_recv() if recv_side else copy.wait_send()

        @pl.when(g > 0)
        def _():
            copy = make(g * gs, gs)
            copy.wait_recv() if recv_side else copy.wait_send()

    partner = {"tp": other}

    def d_copy(g):
        return lambda p, n: remote(
            send.at[pl.ds(pl.multiple_of(p * 16, 16), n * 16)],
            recv.at[core, pl.ds(pl.multiple_of(p * 16, 16), n * 16)],
            d_s.at[g], d_r.at[g], partner,
        )

    def dg_copy(g):
        return lambda p, n: remote(
            gsend.at[pl.ds(p, n)], grecv.at[pl.ds(p, n)], dg_s.at[g], dg_r.at[g], partner
        )

    def r_copy(g):
        return lambda p, n: remote(
            send.at[pl.ds(pl.multiple_of(p * 16, 16), n * 16), 0:fold],
            back.at[pl.ds(pl.multiple_of(p * 16, 16), n * 16)],
            r_s.at[g], r_r.at[g], partner,
        )

    def rg_copy(g):
        return lambda p, n: remote(
            rgs.at[pl.ds(p, n)], bg.at[pl.ds(p, n)], rg_s.at[g], rg_r.at[g], partner
        )

    def expert(g, carry):
        rows_w = wire_rows(g)
        rows_c = pl.ds(pl.multiple_of(g * cr, cr), cr)
        group_wait(g, d_copy(g), True)
        forward = remote(
            recv.at[core, rows_w], recv.at[core, rows_w], f_s, f_r.at[g], partner
        )
        forward.start()
        group_wait(g, dg_copy(g), True)

        def unfold(h):
            for a, into in ((0, xv), (1, yv)):
                tail = jnp.zeros((cr, CH), F32)
                for k in range(nk):
                    piece = recv[h, rows_w, a * fold + k * CH : a * fold + (k + 1) * CH]
                    at = pl.ds(pl.multiple_of(h * half + k * CH, CH), CH)
                    into[rows_c, at] = mm(pm[0], piece).astype(BF16)
                    tail += mm(pm[1 + k], piece)
                at = pl.ds(pl.multiple_of(h * half + fold, CH), CH)
                into[rows_c, at] = tail.astype(BF16)

        unfold(core)
        diff = iota((cr, gs), 0) - CAP * iota((cr, gs), 1)
        inside = (diff >= 0) & (diff < CAP)
        row_src = jnp.where(inside, 1.0, 0.0)
        row_slot = jnp.sum(jnp.where(inside, diff, 0), axis=1, keepdims=True)
        slot_mask = iota((cr, 128), 1) == row_slot
        gate_block = grecv[pl.ds(g * gs, gs)].reshape(gs, 128)
        spread = jnp.dot(row_src, gate_block, preferred_element_type=F32, precision=HI)
        gate = jnp.sum(jnp.where(slot_mask, spread, 0.0), axis=1, keepdims=True)
        forward.wait()
        unfold(other)

        pre = mm(xv[rows_c, :], wgu[...])
        hid_grad = lax.dot_general(yv[rows_c, :], wd[...], NT, preferred_element_type=F32)
        pre_gate, pre_up = pre[:, :ff], pre[:, ff:]
        sig = jax.nn.sigmoid(pre_gate)
        silu = pre_gate * sig
        hidden = (silu * pre_up).astype(BF16).astype(F32)
        gate_part = jnp.sum(hidden * hid_grad, axis=1, keepdims=True)
        scaled = gate * hid_grad
        gp[rows_c, 0:ff] = (scaled * pre_up * sig * (1.0 + pre_gate * (1.0 - sig))).astype(BF16)
        gp[rows_c, ff : 2 * ff] = (scaled * silu).astype(BF16)
        wt[rows_c, :] = (gate * hidden).astype(BF16)
        grads = gp[rows_c, :]
        theirs = wgu[pl.ds(pl.multiple_of(other * half, half), half), :]
        psend[...] = lax.dot_general(grads, theirs, NT, preferred_element_type=F32).astype(BF16)
        gps[...] = lax.dot_general(
            row_src, jnp.where(slot_mask, gate_part, 0.0), TN,
            preferred_element_type=F32, precision=HI,
        )
        swap = remote(psend, precv.at[g], p_s, p_r.at[g], partner)
        swap_gate = remote(gps, gpr.at[g], pg_s, pg_r.at[g], partner)
        swap.start()
        swap_gate.start()
        ours = wgu[pl.ds(pl.multiple_of(core * half, half), half), :]
        own[...] = lax.dot_general(grads, ours, NT, preferred_element_type=F32).astype(BF16)
        group_wait(g, d_copy(g), False)
        swap.wait()
        swap_gate.wait()

        def row_grad(k):
            cols = slice(k * CH, (k + 1) * CH)
            return (own[:, cols].astype(F32) + precv[g, :, cols].astype(F32)).astype(BF16)

        tail = row_grad(nk)
        for k in range(nk):
            part = mm(qm[0], row_grad(k)) + mm(qm[1 + k], tail)
            send[rows_w, k * CH : (k + 1) * CH] = part.astype(BF16)
        rgs[pl.ds(g * gs, gs)] = (gps[...] + gpr[g]).reshape(gs, 1, 128)

        @pl.when(g == 0)
        def _():
            back[0:16, :] = send[0:16, 0:fold]
            bg[0] = rgs[0]

        def start(i, carry):
            p = g * gs + i

            @pl.when(p > 0)
            def _():
                source = {"ep": source_of(p)}
                remote(rgs.at[p], bg.at[p], rg_s.at[g], rg_r.at[g], source).start()
                remote(
                    send.at[block_rows(p), 0:fold], back.at[block_rows(p)],
                    r_s.at[g], r_r.at[g], source,
                ).start()

            return carry

        lax.fori_loop(0, gs, start, 0)
        return carry

    lax.fori_loop(0, ng, expert, 0)

    def grad_gu(i, carry):
        cols = pl.ds(pl.multiple_of(i * CH, CH), CH)
        g = lax.dot_general(xv[:, cols], gp[...], TN, preferred_element_type=F32).astype(BF16)
        wgu[cols, :] = g
        sq = g.astype(F32)
        sq = sq * sq
        ones = jnp.ones((8, ff), F32)
        sqs[0:8, cols] = lax.dot_general(ones, sq[:, :ff], NT, preferred_element_type=F32)
        sqs[8:16, cols] = lax.dot_general(ones, sq[:, ff:], NT, preferred_element_type=F32)
        pltpu.make_async_copy(wgu.at[cols, 0:ff], ggw_o.at[cols, :], st.at[0]).start()
        pltpu.make_async_copy(wgu.at[cols, ff : 2 * ff], guw_o.at[cols, :], st.at[1]).start()
        return carry

    lax.fori_loop(0, width // CH, grad_gu, 0)
    sums = remote(sqs, sqr, sq_s, sq_r, partner)
    sums.start()
    sqa[...] = jnp.zeros_like(sqa)

    def grad_d(i, carry):
        cols = pl.ds(pl.multiple_of(i * CH, CH), CH)
        g = lax.dot_general(wt[...], yv[:, cols], TN, preferred_element_type=F32).astype(BF16)
        wd[:, cols] = g
        sq = g.astype(F32)
        sq = sq * sq
        acc = sq[:, 0:128]
        for k in range(1, CH // 128):
            acc += sq[:, k * 128 : (k + 1) * 128]
        sqa[...] += acc
        pltpu.make_async_copy(wd.at[:, cols], gdw_o.at[:, cols], st.at[2]).start()
        return carry

    lax.fori_loop(0, width // CH, grad_d, 0)
    sq_down = lax.dot_general(
        jnp.ones((8, 128), F32), sqa[...], NT, preferred_element_type=F32, precision=HI
    )
    sqd_o[...] = sq_down[0:1, :] * (1.0 / width)

    lane = iota((rows_tok, 16 * n_pos), 1)
    r = lane & 15
    base = expert_vec(lane >> 4) * 16
    direct = base + r
    folded = jnp.where(r >= CAP, base + r - CAP, -4096)
    homes = [(key_sub[0] == direct) | (key_sub[1] == direct)] + [
        (key_sub[0] == folded + 4 * k) | (key_sub[1] == folded + 4 * k) for k in range(nk)
    ]
    n_wire = 16 * n_pos
    for m in range(nk + 1):
        tokv[m // 2, :, (m % 2) * n_wire : (m % 2 + 1) * n_wire] = hot(homes[m])

    def home(m):
        return tokv[m // 2, :, (m % 2) * n_wire : (m % 2 + 1) * n_wire]

    sums.wait()
    scale = 1.0 / (2 * ff)
    sqg_o[...] = (sqs[0:1, :] + sqr[0:1, :]) * scale
    squ_o[...] = (sqs[8:9, :] + sqr[8:9, :]) * scale

    def arrive(g, carry):
        group_wait(g, rg_copy(g), True)
        group_wait(g, r_copy(g), True)
        return carry

    lax.fori_loop(0, ng, arrive, 0)
    tail = jnp.zeros((rows_tok, CH), F32)
    for k in range(nk):
        piece = back[:, k * CH : (k + 1) * CH]
        gtv[:, k * CH : (k + 1) * CH] = mm(home(0), piece).astype(BF16)
        tail += mm(home(1 + k), piece)
    gtv[:, fold : fold + CH] = tail.astype(BF16)
    out = pltpu.make_async_copy(gtv, gt_o, ld.at[0])
    out.start()
    back_gate = bg[...].reshape(n_pos, 128)
    place = expert_vec(iota((rows_tok, n_pos), 1))
    picked = []
    for j in range(2):
        rows = jnp.dot(
            jnp.where(place == e_sub[j], 1.0, 0.0), back_gate,
            preferred_element_type=F32, precision=HI,
        )
        picked.append(
            jnp.sum(
                jnp.where(iota((rows_tok, 128), 1) == slot_sub[j], rows, 0.0),
                axis=1, keepdims=True,
            )
        )
    gg_o[...] = jnp.where(iota((rows_tok, 2), 1) == 0, picked[0], picked[1])

    def drain(g, carry):
        group_wait(g, dg_copy(g), False)
        group_wait(g, rg_copy(g), False)
        group_wait(g, r_copy(g), False)
        return carry

    lax.fori_loop(0, ng, drain, 0)
    pltpu.make_async_copy(wgu.at[:, 0:ff], ggw_o, st.at[0]).wait()
    pltpu.make_async_copy(wgu.at[:, ff : 2 * ff], guw_o, st.at[1]).wait()
    pltpu.make_async_copy(wd, gdw_o, st.at[2]).wait()
    out.wait()


GS = 16


def body(tokens, cotangent, gates, experts, gate_w, up_w, down_w):
    rows, width = tokens.shape
    half = width // 2
    ff = down_w.shape[1]
    n_pos = SIDE ** 3
    ng = n_pos // GS
    n_wire = 16 * n_pos
    n_rows = CAP * n_pos
    fold = half - CH
    wr, cr = 16 * GS, CAP * GS
    any_spec = pl.BlockSpec(memory_space=pl.ANY)
    vmem = pl.BlockSpec(memory_space=pltpu.VMEM)
    dma = pltpu.SemaphoreType.DMA
    outs = pl.pallas_call(
        functools.partial(kernel, GS),
        out_shape=(
            jax.ShapeDtypeStruct((rows, half), BF16),
            jax.ShapeDtypeStruct((rows, 2), F32),
            jax.ShapeDtypeStruct((width, ff), BF16),
            jax.ShapeDtypeStruct((width, ff), BF16),
            jax.ShapeDtypeStruct((ff, width), BF16),
            jax.ShapeDtypeStruct((1, width), F32),
            jax.ShapeDtypeStruct((1, width), F32),
            jax.ShapeDtypeStruct((1, ff), F32),
        ),
        in_specs=[vmem, vmem, vmem] + [any_spec] * 5,
        out_specs=(any_spec, vmem, any_spec, any_spec, any_spec, vmem, vmem, vmem),
        scratch_shapes=[
            pltpu.VMEM((2, rows, half), BF16),
            pltpu.VMEM((width, 2 * ff), BF16),
            pltpu.VMEM((ff, width), BF16),
            pltpu.VMEM((n_wire, 2 * fold), BF16),
            pltpu.VMEM((2, n_wire, 2 * fold), BF16),
            pltpu.VMEM((n_rows, width), BF16),
            pltpu.VMEM((n_rows, width), BF16),
            pltpu.VMEM((n_rows, 2 * ff), BF16),
            pltpu.VMEM((n_rows, ff), BF16),
            pltpu.VMEM((cr, half), BF16),
            pltpu.VMEM((cr, half), BF16),
            pltpu.VMEM((ng, cr, half), BF16),
            pltpu.VMEM((n_wire, fold), BF16),
            pltpu.VMEM((rows, half), BF16),
            pltpu.VMEM((4, cr, wr), BF16),
            pltpu.VMEM((4, wr, cr), BF16),
            pltpu.VMEM((n_pos, 1, 128), F32),
            pltpu.VMEM((n_pos, 1, 128), F32),
            pltpu.VMEM((GS, 128), F32),
            pltpu.VMEM((ng, GS, 128), F32),
            pltpu.VMEM((n_pos, 1, 128), F32),
            pltpu.VMEM((n_pos, 1, 128), F32),
            pltpu.VMEM((16, width), F32),
            pltpu.VMEM((16, width), F32),
            pltpu.VMEM((ff, 128), F32),
            dma((ng,)), dma((ng,)), dma((ng,)), dma((ng,)),
            dma, dma((ng,)), dma, dma((ng,)), dma, dma((ng,)),
            dma((ng,)), dma((ng,)), dma((ng,)), dma((ng,)),
            dma, dma, dma((5,)), dma((3,)),
        ],
        compiler_params=pltpu.CompilerParams(
            collective_id=0, has_side_effects=True, vmem_limit_bytes=67043328
        ),
    )(experts, experts.T, gates.T, tokens, cotangent, gate_w[0], up_w[0], down_w[0])
    gt, gg, ggw, guw, gdw, sqg, squ, sqd = outs
    return gt, gg, ggw[None], guw[None], gdw[None], sqg, squ, sqd


def solution(mesh):
    placed = (
        P("ep", None),
        P("ep", None),
        P("ep", None),
        P("ep", None),
        P("ep", None, "tp"),
        P("ep", None, "tp"),
        P("ep", "tp", None),
    )
    return jax.shard_map(
        body,
        mesh=mesh,
        in_specs=placed,
        out_specs=(
            P("ep", "tp"),
            P("ep", None),
            P("ep", None, "tp"),
            P("ep", None, "tp"),
            P("ep", "tp", None),
            P("ep", None),
            P("ep", None),
            P("ep", "tp"),
        ),
        check_vma=False,
    )
```

```python
import functools

import jax
import jax.numpy as jnp
from jax import lax
from jax.experimental import pallas as pl
from jax.experimental.pallas import tpu as pltpu
from jax.sharding import PartitionSpec as P

MESH = pl.DeviceIdType.MESH
F32 = jnp.float32
BF16 = jnp.bfloat16
I32 = jnp.int32
CAP = 12
SIDE = 4
CH = 512
NT = (((1,), (1,)), ((), ()))
TN = (((0,), (0,)), ((), ()))
HI = lax.Precision.HIGHEST


def mm(a, b):
    return jnp.dot(a, b, preferred_element_type=F32)


def iota(shape, dim):
    return lax.broadcasted_iota(I32, shape, dim)


def hot(mask):
    return jnp.where(mask, 1.0, 0.0).astype(BF16)


def offsets(p, div, rem):
    q = div(p, 16)
    a = rem(div(p, 8), 2)
    d = rem(div(p, 4), 2)
    oy = rem(p, 4)
    ox = rem(oy + 2 * a + d, 4)
    oz = rem(q + 8 - oy - ox, 4)
    return oz, oy, ox


def scalar_div(a, b):
    return lax.div(a, jnp.int32(b))


def scalar_rem(a, b):
    return lax.rem(a, jnp.int32(b))


def vector_div(a, b):
    return a >> (b.bit_length() - 1)


def vector_rem(a, b):
    return a & (b - 1)


def kernel(
    gs,
    exp_r, gat_r, tok, cot, gw, uw, dw,
    wgu, wd, sqg_o, squ_o, sqd_o, back, bg, tokv, slot_o, place_o,
    send, recv, xv, yv, gp, wt, psend, own, precv, pm, qm,
    gsend, grecv, gps, gpr, rgs, sqs, sqr, sqa,
    d_s, d_r, dg_s, dg_r, f_s, f_r, p_s, p_r, pg_s, pg_r, r_s, r_r, rg_s, rg_r, sq_s, sq_r, ld,
):
    n_pos = SIDE ** 3
    ng = n_pos // gs
    wr = 16 * gs
    cr = CAP * gs
    rows_tok, half = tokv.shape[1], tokv.shape[2]
    width = 2 * half
    fold = half - CH
    nk = fold // CH
    ff = wd.shape[0]
    ep = lax.axis_index("ep")
    core = lax.axis_index("tp")
    other = 1 - core
    cz = scalar_div(ep, 16)
    cy = scalar_rem(scalar_div(ep, 4), 4)
    cx = scalar_rem(ep, 4)

    def offset_at(i):
        oy = i % 4
        return oy, (oy + 2 * (i // 8) + (i // 4) % 2) % 4

    ys = [scalar_rem(cy + o, 4) * 4 for o in range(4)]
    xs = [scalar_rem(cx + o, 4) for o in range(4)]

    def dest_of(g, i):
        oy, ox = offset_at(i)
        return scalar_rem(cz + g + 8 - oy - ox, 4) * 16 + ys[oy] + xs[ox]

    def source_of(g, i):
        oy, ox = offset_at(i)
        return scalar_rem(cz + 4 - g + oy + ox, 4) * 16 + ys[-oy % 4] + xs[-ox % 4]

    def each_peer(g, act):
        for i in range(gs):
            if i == 0:
                pl.when(g > 0)(functools.partial(act, 0))
            else:
                act(i)

    def expert_vec(p):
        oz, oy, ox = offsets(p, vector_div, vector_rem)
        return ((cz + oz) & 3) * 16 + ((cy + oy) & 3) * 4 + ((cx + ox) & 3)

    def remote(src, dst, ssem, rsem, ids):
        return pltpu.make_async_remote_copy(
            src_ref=src, dst_ref=dst, send_sem=ssem, recv_sem=rsem,
            device_id=ids, device_id_type=MESH,
        )

    mine = pl.ds(pl.multiple_of(core * half, half), half)
    loads = [
        pltpu.make_async_copy(tok.at[:, mine], tokv.at[0], ld.at[0]),
        pltpu.make_async_copy(cot.at[:, mine], tokv.at[1], ld.at[1]),
        pltpu.make_async_copy(gw, wgu.at[:, 0:ff], ld.at[2]),
        pltpu.make_async_copy(uw, wgu.at[:, ff : 2 * ff], ld.at[3]),
        pltpu.make_async_copy(dw, wd, ld.at[4]),
    ]
    for copy in loads[:2]:
        copy.start()
    barrier = pltpu.get_barrier_semaphore()

    def greet(g, carry):
        def one(i):
            pl.semaphore_signal(
                barrier, inc=1, device_id={"ep": dest_of(g, i)}, device_id_type=MESH
            )

        each_peer(g, one)
        return carry

    lax.fori_loop(0, ng, greet, 0)
    pl.semaphore_signal(barrier, inc=1, device_id={"tp": other}, device_id_type=MESH)
    e_lane = [exp_r[j : j + 1, :] for j in range(2)]
    hot_t = [
        jnp.where(iota((n_pos, rows_tok), 0) == e_lane[j], 1.0, 0.0).astype(F32) for j in range(2)
    ]
    upper = hot(iota((rows_tok, rows_tok), 0) < iota((rows_tok, rows_tok), 1))
    prior_t = mm((hot_t[0] + hot_t[1]).astype(BF16), upper)
    slot_lane = [
        jnp.sum(hot_t[j] * prior_t, axis=0, keepdims=True).astype(I32) for j in range(2)
    ]
    key_lane = [e_lane[j] * 16 + slot_lane[j] for j in range(2)]
    for j in range(2):
        slot_o[j : j + 1, :] = slot_lane[j]

    place = expert_vec(iota((n_pos, rows_tok), 0))
    gate_rows = jnp.zeros((n_pos, 128), F32)
    for j in range(2):
        place_o[j] = jnp.where(place == e_lane[j], 1.0, 0.0)
        picked = place_o[j] * gat_r[j : j + 1, :]
        slots = jnp.where(iota((128, rows_tok), 0) == slot_lane[j], 1.0, 0.0)
        gate_rows += lax.dot_general(
            picked, slots, NT, preferred_element_type=F32, precision=HI
        )
    gsend[...] = gate_rows.reshape(n_pos, 1, 128)

    loads[0].wait()
    loads[1].wait()
    for copy in loads[2:]:
        copy.start()

    def wire_rows(g):
        return pl.ds(pl.multiple_of(g * wr, wr), wr)

    def block_rows(g, i):
        return pl.ds(pl.multiple_of(g * wr + i * 16, 16), 16)

    def block(g, i, a, dest):
        rows, cols = block_rows(g, i), slice(a * fold, (a + 1) * fold)
        return remote(
            send.at[rows, cols], recv.at[core, rows, cols],
            d_s.at[2 * g + a], d_r.at[2 * g + a], dest,
        )

    def dispatch(g, carry):
        row = iota((wr, rows_tok), 0)
        r = row & 15
        base = expert_vec(g * gs + (row >> 4)) * 16
        direct = base + r
        folded = jnp.where(r >= CAP, base + r - CAP, -4096)
        s_dir = hot((key_lane[0] == direct) | (key_lane[1] == direct))
        s_fold = [
            hot((key_lane[0] == folded + 4 * k) | (key_lane[1] == folded + 4 * k))
            for k in range(nk)
        ]
        for a in range(2):
            last = tokv[a, :, fold : fold + CH]
            for k in range(nk):
                part = mm(s_dir, tokv[a, :, k * CH : (k + 1) * CH]) + mm(s_fold[k], last)
                send[wire_rows(g), a * fold + k * CH : a * fold + (k + 1) * CH] = part.astype(BF16)

        @pl.when(g == 0)
        def _():
            pl.semaphore_wait(barrier, n_pos)
            recv[core, 0:16, :] = send[0:16, :]
            grecv[0] = gsend[0]

        def start(i):
            dest = {"ep": dest_of(g, i)}
            p = g * gs + i
            remote(gsend.at[p], grecv.at[p], dg_s.at[g], dg_r.at[g], dest).start()
            block(g, i, 0, dest).start()

        def start_second(i):
            block(g, i, 1, {"ep": dest_of(g, i)}).start()

        each_peer(g, start)
        each_peer(g, start_second)
        return carry

    lax.fori_loop(0, ng, dispatch, 0)

    to_c, of_w = iota((cr, wr), 0), iota((cr, wr), 1)
    wire_r, wire_s = of_w & 15, of_w >> 4
    pm[0] = hot((wire_r < CAP) & (to_c == CAP * wire_s + wire_r))
    for k in range(nk):
        pm[1 + k] = hot((wire_r >= CAP) & (to_c == CAP * wire_s + 4 * k + wire_r - CAP))
    of_w, to_c = iota((wr, cr), 0), iota((wr, cr), 1)
    wire_r, wire_s = of_w & 15, of_w >> 4
    qm[0] = hot((wire_r < CAP) & (to_c == CAP * wire_s + wire_r))
    for k in range(nk):
        qm[1 + k] = hot((wire_r >= CAP) & (to_c == CAP * wire_s + 4 * k + wire_r - CAP))

    for copy in loads[2:]:
        copy.wait()

    def group_wait(g, make, recv_side):
        @pl.when(g == 0)
        def _():
            copy = make(1, gs - 1)
            copy.wait_recv() if recv_side else copy.wait_send()

        @pl.when(g > 0)
        def _():
            copy = make(g * gs, gs)
            copy.wait_recv() if recv_side else copy.wait_send()

    partner = {"tp": other}

    def d_copy(g, a):
        cols = slice(a * fold, (a + 1) * fold)
        return lambda p, n: remote(
            send.at[pl.ds(pl.multiple_of(p * 16, 16), n * 16), cols],
            recv.at[core, pl.ds(pl.multiple_of(p * 16, 16), n * 16), cols],
            d_s.at[2 * g + a], d_r.at[2 * g + a], partner,
        )

    def dg_copy(g):
        return lambda p, n: remote(
            gsend.at[pl.ds(p, n)], grecv.at[pl.ds(p, n)], dg_s.at[g], dg_r.at[g], partner
        )

    def r_copy(g):
        return lambda p, n: remote(
            send.at[pl.ds(pl.multiple_of(p * 16, 16), n * 16), 0:fold],
            back.at[pl.ds(pl.multiple_of(p * 16, 16), n * 16)],
            r_s.at[g], r_r.at[g], partner,
        )

    def rg_copy(g):
        return lambda p, n: remote(
            rgs.at[pl.ds(p, n)], bg.at[pl.ds(p, n)], rg_s.at[g], rg_r.at[g], partner
        )

    def send_back(g):
        def start(i):
            source = {"ep": source_of(g, i)}
            p = g * gs + i
            remote(rgs.at[p], bg.at[p], rg_s.at[g], rg_r.at[g], source).start()
            remote(
                send.at[block_rows(g, i), 0:fold], back.at[block_rows(g, i)],
                r_s.at[g], r_r.at[g], source,
            ).start()

        each_peer(g, start)

    def expert(g, carry):
        rows_w = wire_rows(g)
        rows_c = pl.ds(pl.multiple_of(g * cr, cr), cr)

        def forward(a):
            cols = slice(a * fold, (a + 1) * fold)
            return remote(
                recv.at[core, rows_w, cols], recv.at[core, rows_w, cols],
                f_s.at[a], f_r.at[2 * g + a], partner,
            )

        def unfold(h, a):
            into = (xv, yv)[a]
            tail = jnp.zeros((cr, CH), F32)
            for k in range(nk):
                piece = recv[h, rows_w, a * fold + k * CH : a * fold + (k + 1) * CH]
                at = pl.ds(pl.multiple_of(h * half + k * CH, CH), CH)
                into[rows_c, at] = mm(pm[0], piece).astype(BF16)
                tail += mm(pm[1 + k], piece)
            at = pl.ds(pl.multiple_of(h * half + fold, CH), CH)
            into[rows_c, at] = tail.astype(BF16)

        def half_of(h):
            return pl.ds(pl.multiple_of(h * half, half), half)

        def pre_half(h):
            return mm(xv[rows_c, half_of(h)], wgu[half_of(h), :])

        def hid_half(h):
            return lax.dot_general(
                yv[rows_c, half_of(h)], wd[:, half_of(h)], NT, preferred_element_type=F32
            )

        group_wait(g, d_copy(g, 0), True)
        forward(0).start()
        unfold(core, 0)
        group_wait(g, d_copy(g, 1), True)
        forward(1).start()
        for at, due in RETURNS:
            @pl.when(g == at)
            def _():
                for other_g in due:
                    send_back(jnp.int32(other_g))

        pre_own = pre_half(core)
        unfold(core, 1)
        hid_own = hid_half(core)
        group_wait(g, dg_copy(g), True)
        diff = iota((cr, gs), 0) - CAP * iota((cr, gs), 1)
        inside = (diff >= 0) & (diff < CAP)
        row_src = jnp.where(inside, 1.0, 0.0)
        row_slot = jnp.sum(jnp.where(inside, diff, 0), axis=1, keepdims=True)
        slot_mask = iota((cr, 128), 1) == row_slot
        gate_block = grecv[pl.ds(g * gs, gs)].reshape(gs, 128)
        spread = jnp.dot(row_src, gate_block, preferred_element_type=F32, precision=HI)
        gate = jnp.sum(jnp.where(slot_mask, spread, 0.0), axis=1, keepdims=True)
        forward(0).wait()
        unfold(other, 0)
        pre = pre_own + pre_half(other)
        forward(1).wait()
        unfold(other, 1)
        hid_grad = hid_own + hid_half(other)
        pre_gate, pre_up = pre[:, :ff], pre[:, ff:]
        sig = jax.nn.sigmoid(pre_gate)
        silu = pre_gate * sig
        hidden = (silu * pre_up).astype(BF16).astype(F32)
        gate_part = jnp.sum(hidden * hid_grad, axis=1, keepdims=True)
        scaled = gate * hid_grad
        gp[rows_c, 0:ff] = (scaled * pre_up * sig * (1.0 + pre_gate * (1.0 - sig))).astype(BF16)
        gp[rows_c, ff : 2 * ff] = (scaled * silu).astype(BF16)
        wt[rows_c, :] = (gate * hidden).astype(BF16)
        grads = gp[rows_c, :]
        theirs = wgu[pl.ds(pl.multiple_of(other * half, half), half), :]
        psend[...] = lax.dot_general(grads, theirs, NT, preferred_element_type=F32).astype(BF16)
        swap = remote(psend, precv.at[g], p_s, p_r.at[g], partner)
        swap.start()
        gps[...] = lax.dot_general(
            row_src, jnp.where(slot_mask, gate_part, 0.0), TN,
            preferred_element_type=F32, precision=HI,
        )
        swap_gate = remote(gps, gpr.at[g], pg_s, pg_r.at[g], partner)
        swap_gate.start()
        ours = wgu[pl.ds(pl.multiple_of(core * half, half), half), :]
        own[...] = lax.dot_general(grads, ours, NT, preferred_element_type=F32).astype(BF16)
        group_wait(g, d_copy(g, 0), False)
        group_wait(g, d_copy(g, 1), False)
        swap.wait()
        swap_gate.wait()

        def row_grad(k):
            cols = slice(k * CH, (k + 1) * CH)
            return (own[:, cols].astype(F32) + precv[g, :, cols].astype(F32)).astype(BF16)

        tail = row_grad(nk)
        for k in range(nk):
            part = mm(qm[0], row_grad(k)) + mm(qm[1 + k], tail)
            send[rows_w, k * CH : (k + 1) * CH] = part.astype(BF16)
        rgs[pl.ds(g * gs, gs)] = (gps[...] + gpr[g]).reshape(gs, 1, 128)

        @pl.when(g == 0)
        def _():
            back[0:16, :] = send[0:16, 0:fold]
            bg[0] = rgs[0]

        @pl.when(g == ng - 1)
        def _():
            send_back(g)

        return carry

    lax.fori_loop(0, ng, expert, 0)

    def grad_gu(i, carry):
        cols = pl.ds(pl.multiple_of(i * CH, CH), CH)
        g = lax.dot_general(xv[:, cols], gp[...], TN, preferred_element_type=F32).astype(BF16)
        wgu[cols, :] = g
        sq = g.astype(F32)
        sq = sq * sq
        ones = jnp.ones((8, ff), F32)
        sqs[0:8, cols] = lax.dot_general(ones, sq[:, :ff], NT, preferred_element_type=F32)
        sqs[8:16, cols] = lax.dot_general(ones, sq[:, ff:], NT, preferred_element_type=F32)
        return carry

    lax.fori_loop(0, width // CH, grad_gu, 0)
    sums = remote(sqs, sqr, sq_s, sq_r, partner)
    sums.start()
    sqa[...] = jnp.zeros_like(sqa)

    def grad_d(i, carry):
        cols = pl.ds(pl.multiple_of(i * CH, CH), CH)
        g = lax.dot_general(wt[...], yv[:, cols], TN, preferred_element_type=F32).astype(BF16)
        wd[:, cols] = g
        sq = g.astype(F32)
        sq = sq * sq
        acc = sq[:, 0:128]
        for k in range(1, CH // 128):
            acc += sq[:, k * 128 : (k + 1) * 128]
        sqa[...] += acc
        return carry

    lax.fori_loop(0, width // CH, grad_d, 0)
    sq_down = lax.dot_general(
        jnp.ones((8, 128), F32), sqa[...], NT, preferred_element_type=F32, precision=HI
    )
    sqd_o[...] = sq_down[0:1, :] * (1.0 / width)

    hot_c = [
        jnp.transpose(
            jnp.where(iota((n_pos, rows_tok), 0) == exp_r[j : j + 1, :], 1.0, 0.0)
        )
        for j in range(2)
    ]
    lower = hot(iota((rows_tok, rows_tok), 1) < iota((rows_tok, rows_tok), 0))
    prior_c = mm(lower, (hot_c[0] + hot_c[1]).astype(BF16))
    key_sub = [
        jnp.sum(
            hot_c[j] * (prior_c + 16.0 * iota((rows_tok, n_pos), 1).astype(F32)),
            axis=1, keepdims=True,
        ).astype(I32)
        for j in range(2)
    ]
    lane = iota((rows_tok, 16 * n_pos), 1)
    r = lane & 15
    base = expert_vec(lane >> 4) * 16
    direct = base + r
    folded = jnp.where(r >= CAP, base + r - CAP, -4096)
    homes = [(key_sub[0] == direct) | (key_sub[1] == direct)] + [
        (key_sub[0] == folded + 4 * k) | (key_sub[1] == folded + 4 * k) for k in range(nk)
    ]
    n_wire = 16 * n_pos
    for m in range(nk + 1):
        tokv[m // 2, :, (m % 2) * n_wire : (m % 2 + 1) * n_wire] = hot(homes[m])

    sums.wait()
    scale = 1.0 / (2 * ff)
    sqg_o[...] = (sqs[0:1, :] + sqr[0:1, :]) * scale
    squ_o[...] = (sqs[8:9, :] + sqr[8:9, :]) * scale

    def arrive(g, carry):
        group_wait(g, rg_copy(g), True)
        group_wait(g, r_copy(g), True)
        return carry

    lax.fori_loop(0, ng, arrive, 0)
    def drain(g, carry):
        group_wait(g, dg_copy(g), False)
        group_wait(g, rg_copy(g), False)
        group_wait(g, r_copy(g), False)
        return carry

    lax.fori_loop(0, ng, drain, 0)


def flush(
    wgu, wd, sqg, squ, sqd, back, bg, homes, slot, place,
    gt_o, gg_o, ggw_o, guw_o, gdw_o, sqg_o, squ_o, sqd_o, gtv, sem,
):
    ff = wd.shape[0]
    rows_tok = gtv.shape[0]
    n_wire, fold = back.shape
    nk = fold // CH
    part = wgu.shape[0] // 4
    pairs = [
        (wgu.at[i * part : (i + 1) * part, j * ff : (j + 1) * ff],
         (ggw_o, guw_o)[j].at[i * part : (i + 1) * part, :])
        for i in range(4) for j in range(2)
    ] + [
        (wd.at[i * (ff // 4) : (i + 1) * (ff // 4), :],
         gdw_o.at[i * (ff // 4) : (i + 1) * (ff // 4), :])
        for i in range(4)
    ] + [(sqg, sqg_o), (squ, squ_o), (sqd, sqd_o), (gtv, gt_o)]
    copies = [
        pltpu.make_async_copy(src, dst, sem.at[i]) for i, (src, dst) in enumerate(pairs)
    ]
    for copy in copies[:-1]:
        copy.start()

    def home(m):
        return homes[m // 2, :, (m % 2) * n_wire : (m % 2 + 1) * n_wire]

    tail = jnp.zeros((rows_tok, CH), F32)
    for k in range(nk):
        piece = back[:, k * CH : (k + 1) * CH]
        gtv[:, k * CH : (k + 1) * CH] = mm(home(0), piece).astype(BF16)
        tail += mm(home(1 + k), piece)
    gtv[:, fold : fold + CH] = tail.astype(BF16)
    copies[-1].start()
    back_gate = bg[...].reshape(bg.shape[0], 128)
    for j in range(2):
        rows = lax.dot_general(
            back_gate, place[j], TN, preferred_element_type=F32, precision=HI
        )
        gg_o[j : j + 1, :] = jnp.sum(
            jnp.where(iota((128, rows_tok), 0) == slot[j : j + 1, :], rows, 0.0),
            axis=0, keepdims=True,
        )
    for copy in copies:
        copy.wait()


GS = 16
RETURNS = ((3, (0, 1, 2)),)
VMEM_K1 = 48 * 2**20
VMEM_K2 = 6 * 2**20


def body(tokens, cotangent, gates, experts, gate_w, up_w, down_w):
    rows, width = tokens.shape
    half = width // 2
    ff = down_w.shape[1]
    n_pos = SIDE ** 3
    ng = n_pos // GS
    n_wire = 16 * n_pos
    n_rows = CAP * n_pos
    fold = half - CH
    wr, cr = 16 * GS, CAP * GS
    any_spec = pl.BlockSpec(memory_space=pl.ANY)
    vmem = pl.BlockSpec(memory_space=pltpu.VMEM)
    dma = pltpu.SemaphoreType.DMA
    outs = pl.pallas_call(
        functools.partial(kernel, GS),
        out_shape=(
            pltpu.VMEM((width, 2 * ff), BF16),
            pltpu.VMEM((ff, width), BF16),
            pltpu.VMEM((1, width), F32),
            pltpu.VMEM((1, width), F32),
            pltpu.VMEM((1, ff), F32),
            pltpu.VMEM((n_wire, fold), BF16),
            pltpu.VMEM((n_pos, 1, 128), F32),
            pltpu.VMEM((2, rows, half), BF16),
            pltpu.VMEM((2, rows), I32),
            pltpu.VMEM((2, n_pos, rows), F32),
        ),
        in_specs=[vmem, vmem] + [any_spec] * 5,
        out_specs=(vmem,) * 10,
        scratch_shapes=[
            pltpu.VMEM((n_wire, 2 * fold), BF16),
            pltpu.VMEM((2, n_wire, 2 * fold), BF16),
            pltpu.VMEM((n_rows, width), BF16),
            pltpu.VMEM((n_rows, width), BF16),
            pltpu.VMEM((n_rows, 2 * ff), BF16),
            pltpu.VMEM((n_rows, ff), BF16),
            pltpu.VMEM((cr, half), BF16),
            pltpu.VMEM((cr, half), BF16),
            pltpu.VMEM((ng, cr, half), BF16),
            pltpu.VMEM((4, cr, wr), BF16),
            pltpu.VMEM((4, wr, cr), BF16),
            pltpu.VMEM((n_pos, 1, 128), F32),
            pltpu.VMEM((n_pos, 1, 128), F32),
            pltpu.VMEM((GS, 128), F32),
            pltpu.VMEM((ng, GS, 128), F32),
            pltpu.VMEM((n_pos, 1, 128), F32),
            pltpu.VMEM((16, width), F32),
            pltpu.VMEM((16, width), F32),
            pltpu.VMEM((ff, 128), F32),
            dma((2 * ng,)), dma((2 * ng,)), dma((ng,)), dma((ng,)),
            dma((2,)), dma((2 * ng,)), dma, dma((ng,)), dma, dma((ng,)),
            dma((ng,)), dma((ng,)), dma((ng,)), dma((ng,)),
            dma, dma, dma((5,)),
        ],
        compiler_params=pltpu.CompilerParams(
            collective_id=0, has_side_effects=True, vmem_limit_bytes=VMEM_K1
        ),
    )(experts.T, gates.T, tokens, cotangent, gate_w[0], up_w[0], down_w[0])
    outs = pl.pallas_call(
        flush,
        out_shape=(
            jax.ShapeDtypeStruct((rows, half), BF16),
            jax.ShapeDtypeStruct((2, rows), F32),
            jax.ShapeDtypeStruct((width, ff), BF16),
            jax.ShapeDtypeStruct((width, ff), BF16),
            jax.ShapeDtypeStruct((ff, width), BF16),
            jax.ShapeDtypeStruct((1, width), F32),
            jax.ShapeDtypeStruct((1, width), F32),
            jax.ShapeDtypeStruct((1, ff), F32),
        ),
        in_specs=[vmem] * 10,
        out_specs=(any_spec, vmem) + (any_spec,) * 6,
        scratch_shapes=[pltpu.VMEM((rows, half), BF16), dma((16,))],
        compiler_params=pltpu.CompilerParams(vmem_limit_bytes=VMEM_K2),
    )(*outs)
    gt, gg, ggw, guw, gdw, sqg, squ, sqd = outs
    return gt, gg.T, ggw[None], guw[None], gdw[None], sqg, squ, sqd


def solution(mesh):
    placed = (
        P("ep", None),
        P("ep", None),
        P("ep", None),
        P("ep", None),
        P("ep", None, "tp"),
        P("ep", None, "tp"),
        P("ep", "tp", None),
    )
    return jax.shard_map(
        body,
        mesh=mesh,
        in_specs=placed,
        out_specs=(
            P("ep", "tp"),
            P("ep", None),
            P("ep", None, "tp"),
            P("ep", None, "tp"),
            P("ep", "tp", None),
            P("ep", None),
            P("ep", None),
            P("ep", "tp"),
        ),
        check_vma=False,
    )
```

```python
import functools

import jax
import jax.numpy as jnp
from jax import lax
from jax.experimental import pallas as pl
from jax.experimental.pallas import tpu as pltpu
from jax.sharding import PartitionSpec as P

MESH = pl.DeviceIdType.MESH
F32 = jnp.float32
BF16 = jnp.bfloat16
I32 = jnp.int32
CAP = 12
SIDE = 4
CH = 512
NT = (((1,), (1,)), ((), ()))
TN = (((0,), (0,)), ((), ()))
HI = lax.Precision.HIGHEST


def mm(a, b):
    return jnp.dot(a, b, preferred_element_type=F32)


def iota(shape, dim):
    return lax.broadcasted_iota(I32, shape, dim)


def hot(mask):
    return jnp.where(mask, 1.0, 0.0).astype(BF16)


def offsets(p, div, rem):
    q = div(p, 16)
    a = rem(div(p, 8), 2)
    d = rem(div(p, 4), 2)
    oy = rem(p, 4)
    ox = rem(oy + 2 * a + d, 4)
    oz = rem(q + 8 - oy - ox, 4)
    return oz, oy, ox


def scalar_div(a, b):
    return lax.div(a, jnp.int32(b))


def scalar_rem(a, b):
    return lax.rem(a, jnp.int32(b))


def vector_div(a, b):
    return a >> (b.bit_length() - 1)


def vector_rem(a, b):
    return a & (b - 1)


def kernel(
    gs,
    exp_r, gat_r, tok, cot, gw, uw, dw,
    wgu, wd, sqg_o, squ_o, sqd_o, back, bg, tokv, slot_o, place_o,
    send, recv, xv, yv, gp, wt, psend, own, precv, pm, qm,
    gsend, grecv, gps, gpr, rgs, sqs, sqr, sqa,
    d_s, d_r, dg_s, dg_r, f_s, f_r, p_s, p_r, pg_s, pg_r, r_s, r_r, rg_s, rg_r, sq_s, sq_r, ld,
):
    n_pos = SIDE ** 3
    ng = n_pos // gs
    wr = 16 * gs
    cr = CAP * gs
    rows_tok, half = tokv.shape[1], tokv.shape[2]
    width = 2 * half
    fold = half - CH
    nk = fold // CH
    ff = wd.shape[0]
    ep = lax.axis_index("ep")
    core = lax.axis_index("tp")
    other = 1 - core
    cz = scalar_div(ep, 16)
    cy = scalar_rem(scalar_div(ep, 4), 4)
    cx = scalar_rem(ep, 4)

    def offset_at(i):
        oy = i % 4
        return oy, (oy + 2 * (i // 8) + (i // 4) % 2) % 4

    ys = [scalar_rem(cy + o, 4) * 4 for o in range(4)]
    xs = [scalar_rem(cx + o, 4) for o in range(4)]

    def dest_of(g, i):
        oy, ox = offset_at(i)
        return scalar_rem(cz + g + 8 - oy - ox, 4) * 16 + ys[oy] + xs[ox]

    def source_of(g, i):
        oy, ox = offset_at(i)
        return scalar_rem(cz + 4 - g + oy + ox, 4) * 16 + ys[-oy % 4] + xs[-ox % 4]

    def each_peer(g, act):
        for i in range(gs):
            if i == 0:
                pl.when(g > 0)(functools.partial(act, 0))
            else:
                act(i)

    def expert_vec(p):
        oz, oy, ox = offsets(p, vector_div, vector_rem)
        return ((cz + oz) & 3) * 16 + ((cy + oy) & 3) * 4 + ((cx + ox) & 3)

    def remote(src, dst, ssem, rsem, ids):
        return pltpu.make_async_remote_copy(
            src_ref=src, dst_ref=dst, send_sem=ssem, recv_sem=rsem,
            device_id=ids, device_id_type=MESH,
        )

    mine = pl.ds(pl.multiple_of(core * half, half), half)
    loads = [
        pltpu.make_async_copy(tok.at[:, mine], tokv.at[0], ld.at[0]),
        pltpu.make_async_copy(cot.at[:, mine], tokv.at[1], ld.at[1]),
        pltpu.make_async_copy(gw, wgu.at[:, 0:ff], ld.at[2]),
        pltpu.make_async_copy(uw, wgu.at[:, ff : 2 * ff], ld.at[3]),
        pltpu.make_async_copy(dw, wd, ld.at[4]),
    ]
    for copy in loads[:2]:
        copy.start()
    barrier = pltpu.get_barrier_semaphore()

    def greet(g, carry):
        def one(i):
            pl.semaphore_signal(
                barrier, inc=1, device_id={"ep": dest_of(g, i)}, device_id_type=MESH
            )

        each_peer(g, one)
        return carry

    lax.fori_loop(0, ng, greet, 0)
    pl.semaphore_signal(barrier, inc=1, device_id={"tp": other}, device_id_type=MESH)
    e_lane = [exp_r[j : j + 1, :] for j in range(2)]
    hot_t = [
        jnp.where(iota((n_pos, rows_tok), 0) == e_lane[j], 1.0, 0.0).astype(F32) for j in range(2)
    ]
    upper = hot(iota((rows_tok, rows_tok), 0) < iota((rows_tok, rows_tok), 1))
    prior_t = mm((hot_t[0] + hot_t[1]).astype(BF16), upper)
    slot_lane = [
        jnp.sum(hot_t[j] * prior_t, axis=0, keepdims=True).astype(I32) for j in range(2)
    ]
    key_lane = [e_lane[j] * 16 + slot_lane[j] for j in range(2)]
    for j in range(2):
        slot_o[j : j + 1, :] = slot_lane[j]

    place = expert_vec(iota((n_pos, rows_tok), 0))
    gate_rows = jnp.zeros((n_pos, 128), F32)
    for j in range(2):
        place_o[j] = jnp.where(place == e_lane[j], 1.0, 0.0)
        picked = place_o[j] * gat_r[j : j + 1, :]
        slots = jnp.where(iota((128, rows_tok), 0) == slot_lane[j], 1.0, 0.0)
        gate_rows += lax.dot_general(
            picked, slots, NT, preferred_element_type=F32, precision=HI
        )
    gsend[...] = gate_rows.reshape(n_pos, 1, 128)

    loads[0].wait()
    loads[1].wait()
    for copy in loads[2:]:
        copy.start()

    def wire_rows(g):
        return pl.ds(pl.multiple_of(g * wr, wr), wr)

    def block_rows(g, i):
        return pl.ds(pl.multiple_of(g * wr + i * 16, 16), 16)

    def block(g, i, a, dest):
        rows, cols = block_rows(g, i), slice(a * fold, (a + 1) * fold)
        return remote(
            send.at[rows, cols], recv.at[core, rows, cols],
            d_s.at[2 * g + a], d_r.at[2 * g + a], dest,
        )

    def dispatch(g, carry):
        row = iota((wr, rows_tok), 0)
        r = row & 15
        base = expert_vec(g * gs + (row >> 4)) * 16
        direct = base + r
        folded = jnp.where(r >= CAP, base + r - CAP, -4096)
        s_dir = hot((key_lane[0] == direct) | (key_lane[1] == direct))
        s_fold = [
            hot((key_lane[0] == folded + 4 * k) | (key_lane[1] == folded + 4 * k))
            for k in range(nk)
        ]
        for a in range(2):
            last = tokv[a, :, fold : fold + CH]
            for k in range(nk):
                part = mm(s_dir, tokv[a, :, k * CH : (k + 1) * CH]) + mm(s_fold[k], last)
                send[wire_rows(g), a * fold + k * CH : a * fold + (k + 1) * CH] = part.astype(BF16)

        @pl.when(g == 0)
        def _():
            pl.semaphore_wait(barrier, n_pos)
            recv[core, 0:16, :] = send[0:16, :]
            grecv[0] = gsend[0]

        def start(i):
            dest = {"ep": dest_of(g, i)}
            p = g * gs + i
            remote(gsend.at[p], grecv.at[p], dg_s.at[g], dg_r.at[g], dest).start()
            block(g, i, 0, dest).start()

        def start_second(i):
            block(g, i, 1, {"ep": dest_of(g, i)}).start()

        each_peer(g, start)
        each_peer(g, start_second)
        return carry

    lax.fori_loop(0, ng, dispatch, 0)

    to_c, of_w = iota((cr, wr), 0), iota((cr, wr), 1)
    wire_r, wire_s = of_w & 15, of_w >> 4
    pm[0] = hot((wire_r < CAP) & (to_c == CAP * wire_s + wire_r))
    for k in range(nk):
        pm[1 + k] = hot((wire_r >= CAP) & (to_c == CAP * wire_s + 4 * k + wire_r - CAP))
    of_w, to_c = iota((wr, cr), 0), iota((wr, cr), 1)
    wire_r, wire_s = of_w & 15, of_w >> 4
    qm[0] = hot((wire_r < CAP) & (to_c == CAP * wire_s + wire_r))
    for k in range(nk):
        qm[1 + k] = hot((wire_r >= CAP) & (to_c == CAP * wire_s + 4 * k + wire_r - CAP))

    for copy in loads[2:]:
        copy.wait()

    def group_wait(g, make, recv_side):
        @pl.when(g == 0)
        def _():
            copy = make(1, gs - 1)
            copy.wait_recv() if recv_side else copy.wait_send()

        @pl.when(g > 0)
        def _():
            copy = make(g * gs, gs)
            copy.wait_recv() if recv_side else copy.wait_send()

    partner = {"tp": other}

    def d_copy(g, a):
        cols = slice(a * fold, (a + 1) * fold)
        return lambda p, n: remote(
            send.at[pl.ds(pl.multiple_of(p * 16, 16), n * 16), cols],
            recv.at[core, pl.ds(pl.multiple_of(p * 16, 16), n * 16), cols],
            d_s.at[2 * g + a], d_r.at[2 * g + a], partner,
        )

    def dg_copy(g):
        return lambda p, n: remote(
            gsend.at[pl.ds(p, n)], grecv.at[pl.ds(p, n)], dg_s.at[g], dg_r.at[g], partner
        )

    def r_copy(g):
        return lambda p, n: remote(
            send.at[pl.ds(pl.multiple_of(p * 16, 16), n * 16), 0:fold],
            back.at[pl.ds(pl.multiple_of(p * 16, 16), n * 16)],
            r_s.at[g], r_r.at[g], partner,
        )

    def rg_copy(g):
        return lambda p, n: remote(
            rgs.at[pl.ds(p, n)], bg.at[pl.ds(p, n)], rg_s.at[g], rg_r.at[g], partner
        )

    def send_back(g):
        def start(i):
            source = {"ep": source_of(g, i)}
            p = g * gs + i
            remote(rgs.at[p], bg.at[p], rg_s.at[g], rg_r.at[g], source).start()
            remote(
                send.at[block_rows(g, i), 0:fold], back.at[block_rows(g, i)],
                r_s.at[g], r_r.at[g], source,
            ).start()

        each_peer(g, start)

    def expert(g, carry):
        rows_w = wire_rows(g)
        rows_c = pl.ds(pl.multiple_of(g * cr, cr), cr)

        def forward(a):
            cols = slice(a * fold, (a + 1) * fold)
            return remote(
                recv.at[core, rows_w, cols], recv.at[core, rows_w, cols],
                f_s.at[a], f_r.at[2 * g + a], partner,
            )

        def unfold(h, a):
            into = (xv, yv)[a]
            tail = jnp.zeros((cr, CH), F32)
            for k in range(nk):
                piece = recv[h, rows_w, a * fold + k * CH : a * fold + (k + 1) * CH]
                at = pl.ds(pl.multiple_of(h * half + k * CH, CH), CH)
                into[rows_c, at] = mm(pm[0], piece).astype(BF16)
                tail += mm(pm[1 + k], piece)
            at = pl.ds(pl.multiple_of(h * half + fold, CH), CH)
            into[rows_c, at] = tail.astype(BF16)

        def half_of(h):
            return pl.ds(pl.multiple_of(h * half, half), half)

        def pre_half(h):
            return mm(xv[rows_c, half_of(h)], wgu[half_of(h), :])

        def hid_half(h):
            return lax.dot_general(
                yv[rows_c, half_of(h)], wd[:, half_of(h)], NT, preferred_element_type=F32
            )

        group_wait(g, d_copy(g, 0), True)
        forward(0).start()
        unfold(core, 0)
        group_wait(g, d_copy(g, 1), True)
        forward(1).start()
        for at, due in RETURNS:
            @pl.when(g == at)
            def _():
                for other_g in due:
                    send_back(jnp.int32(other_g))

        pre_own = pre_half(core)
        unfold(core, 1)
        hid_own = hid_half(core)
        group_wait(g, dg_copy(g), True)
        diff = iota((cr, gs), 0) - CAP * iota((cr, gs), 1)
        inside = (diff >= 0) & (diff < CAP)
        row_src = jnp.where(inside, 1.0, 0.0)
        row_slot = jnp.sum(jnp.where(inside, diff, 0), axis=1, keepdims=True)
        slot_mask = iota((cr, 128), 1) == row_slot
        gate_block = grecv[pl.ds(g * gs, gs)].reshape(gs, 128)
        spread = jnp.dot(row_src, gate_block, preferred_element_type=F32, precision=HI)
        gate = jnp.sum(jnp.where(slot_mask, spread, 0.0), axis=1, keepdims=True)
        forward(0).wait()
        unfold(other, 0)
        pre = pre_own + pre_half(other)
        forward(1).wait()
        unfold(other, 1)
        hid_grad = hid_own + hid_half(other)
        pre_gate, pre_up = pre[:, :ff], pre[:, ff:]
        sig = jax.nn.sigmoid(pre_gate)
        silu = pre_gate * sig
        hidden = (silu * pre_up).astype(BF16).astype(F32)
        gate_part = jnp.sum(hidden * hid_grad, axis=1, keepdims=True)
        scaled = gate * hid_grad
        gp[rows_c, 0:ff] = (scaled * pre_up * sig * (1.0 + pre_gate * (1.0 - sig))).astype(BF16)
        gp[rows_c, ff : 2 * ff] = (scaled * silu).astype(BF16)
        wt[rows_c, :] = (gate * hidden).astype(BF16)
        grads = gp[rows_c, :]
        theirs = wgu[pl.ds(pl.multiple_of(other * half, half), half), :]
        psend[...] = lax.dot_general(grads, theirs, NT, preferred_element_type=F32).astype(BF16)
        swap = remote(psend, precv.at[g], p_s, p_r.at[g], partner)
        swap.start()
        gps[...] = lax.dot_general(
            row_src, jnp.where(slot_mask, gate_part, 0.0), TN,
            preferred_element_type=F32, precision=HI,
        )
        swap_gate = remote(gps, gpr.at[g], pg_s, pg_r.at[g], partner)
        swap_gate.start()
        ours = wgu[pl.ds(pl.multiple_of(core * half, half), half), :]
        own[...] = lax.dot_general(grads, ours, NT, preferred_element_type=F32).astype(BF16)
        group_wait(g, d_copy(g, 0), False)
        group_wait(g, d_copy(g, 1), False)
        swap.wait()
        swap_gate.wait()

        def row_grad(k):
            cols = slice(k * CH, (k + 1) * CH)
            return (own[:, cols].astype(F32) + precv[g, :, cols].astype(F32)).astype(BF16)

        tail = row_grad(nk)
        for k in range(nk):
            part = mm(qm[0], row_grad(k)) + mm(qm[1 + k], tail)
            send[rows_w, k * CH : (k + 1) * CH] = part.astype(BF16)
        rgs[pl.ds(g * gs, gs)] = (gps[...] + gpr[g]).reshape(gs, 1, 128)

        @pl.when(g == 0)
        def _():
            back[0:16, :] = send[0:16, 0:fold]
            bg[0] = rgs[0]

        @pl.when(g == ng - 1)
        def _():
            send_back(g)

        return carry

    lax.fori_loop(0, ng, expert, 0)

    def grad_gu(i, carry):
        cols = pl.ds(pl.multiple_of(i * CH, CH), CH)
        g = lax.dot_general(xv[:, cols], gp[...], TN, preferred_element_type=F32).astype(BF16)
        wgu[cols, :] = g
        sq = g.astype(F32)
        sq = sq * sq
        ones = jnp.ones((8, ff), F32)
        sqs[0:8, cols] = lax.dot_general(ones, sq[:, :ff], NT, preferred_element_type=F32)
        sqs[8:16, cols] = lax.dot_general(ones, sq[:, ff:], NT, preferred_element_type=F32)
        return carry

    lax.fori_loop(0, width // CH, grad_gu, 0)
    sums = remote(sqs, sqr, sq_s, sq_r, partner)
    sums.start()
    sqa[...] = jnp.zeros_like(sqa)

    def grad_d(i, carry):
        cols = pl.ds(pl.multiple_of(i * CH, CH), CH)
        g = lax.dot_general(wt[...], yv[:, cols], TN, preferred_element_type=F32).astype(BF16)
        wd[:, cols] = g
        sq = g.astype(F32)
        sq = sq * sq
        acc = sq[:, 0:128]
        for k in range(1, CH // 128):
            acc += sq[:, k * 128 : (k + 1) * 128]
        sqa[...] += acc
        return carry

    lax.fori_loop(0, width // CH, grad_d, 0)
    sq_down = lax.dot_general(
        jnp.ones((8, 128), F32), sqa[...], NT, preferred_element_type=F32, precision=HI
    )
    sqd_o[...] = sq_down[0:1, :] * (1.0 / width)

    hot_c = [
        jnp.transpose(
            jnp.where(iota((n_pos, rows_tok), 0) == exp_r[j : j + 1, :], 1.0, 0.0)
        )
        for j in range(2)
    ]
    lower = hot(iota((rows_tok, rows_tok), 1) < iota((rows_tok, rows_tok), 0))
    prior_c = mm(lower, (hot_c[0] + hot_c[1]).astype(BF16))
    key_sub = [
        jnp.sum(
            hot_c[j] * (prior_c + 16.0 * iota((rows_tok, n_pos), 1).astype(F32)),
            axis=1, keepdims=True,
        ).astype(I32)
        for j in range(2)
    ]
    lane = iota((rows_tok, 16 * n_pos), 1)
    r = lane & 15
    base = expert_vec(lane >> 4) * 16
    direct = base + r
    folded = jnp.where(r >= CAP, base + r - CAP, -4096)
    homes = [(key_sub[0] == direct) | (key_sub[1] == direct)] + [
        (key_sub[0] == folded + 4 * k) | (key_sub[1] == folded + 4 * k) for k in range(nk)
    ]
    n_wire = 16 * n_pos
    for m in range(nk + 1):
        tokv[m // 2, :, (m % 2) * n_wire : (m % 2 + 1) * n_wire] = hot(homes[m])

    sums.wait()
    scale = 1.0 / (2 * ff)
    sqg_o[...] = (sqs[0:1, :] + sqr[0:1, :]) * scale
    squ_o[...] = (sqs[8:9, :] + sqr[8:9, :]) * scale

    def arrive(g, carry):
        group_wait(g, rg_copy(g), True)
        group_wait(g, r_copy(g), True)
        return carry

    lax.fori_loop(0, ng, arrive, 0)
    def drain(g, carry):
        group_wait(g, dg_copy(g), False)
        group_wait(g, rg_copy(g), False)
        group_wait(g, r_copy(g), False)
        return carry

    lax.fori_loop(0, ng, drain, 0)


def flush(
    wgu, wd, sqg, squ, sqd, back, bg, homes, slot, place,
    gt_o, gg_o, ggw_o, guw_o, gdw_o, sqg_o, squ_o, sqd_o, gtv, sem,
):
    ff = wd.shape[0]
    rows_tok = gtv.shape[0]
    n_wire, fold = back.shape
    nk = fold // CH
    part = wgu.shape[0] // 4
    pairs = [
        (wgu.at[i * part : (i + 1) * part, j * ff : (j + 1) * ff],
         (ggw_o, guw_o)[j].at[i * part : (i + 1) * part, :])
        for i in range(4) for j in range(2)
    ] + [
        (wd.at[i * (ff // 4) : (i + 1) * (ff // 4), :],
         gdw_o.at[i * (ff // 4) : (i + 1) * (ff // 4), :])
        for i in range(4)
    ] + [(sqg, sqg_o), (squ, squ_o), (sqd, sqd_o)] + [
        (gtv.at[:, k * CH : (k + 1) * CH], gt_o.at[:, k * CH : (k + 1) * CH])
        for k in range(nk + 1)
    ]
    copies = [
        pltpu.make_async_copy(src, dst, sem.at[i]) for i, (src, dst) in enumerate(pairs)
    ]
    for copy in copies[: -nk - 1]:
        copy.start()

    def home(m):
        return homes[m // 2, :, (m % 2) * n_wire : (m % 2 + 1) * n_wire]

    tail = jnp.zeros((rows_tok, CH), F32)
    for k in range(nk):
        piece = back[:, k * CH : (k + 1) * CH]
        gtv[:, k * CH : (k + 1) * CH] = mm(home(0), piece).astype(BF16)
        tail += mm(home(1 + k), piece)
        copies[k - nk - 1].start()
    gtv[:, fold : fold + CH] = tail.astype(BF16)
    copies[-1].start()
    back_gate = bg[...].reshape(bg.shape[0], 128)
    for j in range(2):
        rows = lax.dot_general(
            back_gate, place[j], TN, preferred_element_type=F32, precision=HI
        )
        gg_o[j : j + 1, :] = jnp.sum(
            jnp.where(iota((128, rows_tok), 0) == slot[j : j + 1, :], rows, 0.0),
            axis=0, keepdims=True,
        )
    for copy in copies:
        copy.wait()


GS = 16
RETURNS = ((3, (0, 1, 2)),)
VMEM_K1 = 48 * 2**20
VMEM_K2 = 6 * 2**20


def body(tokens, cotangent, gates, experts, gate_w, up_w, down_w):
    rows, width = tokens.shape
    half = width // 2
    ff = down_w.shape[1]
    n_pos = SIDE ** 3
    ng = n_pos // GS
    n_wire = 16 * n_pos
    n_rows = CAP * n_pos
    fold = half - CH
    wr, cr = 16 * GS, CAP * GS
    any_spec = pl.BlockSpec(memory_space=pl.ANY)
    vmem = pl.BlockSpec(memory_space=pltpu.VMEM)
    dma = pltpu.SemaphoreType.DMA
    outs = pl.pallas_call(
        functools.partial(kernel, GS),
        out_shape=(
            pltpu.VMEM((width, 2 * ff), BF16),
            pltpu.VMEM((ff, width), BF16),
            pltpu.VMEM((1, width), F32),
            pltpu.VMEM((1, width), F32),
            pltpu.VMEM((1, ff), F32),
            pltpu.VMEM((n_wire, fold), BF16),
            pltpu.VMEM((n_pos, 1, 128), F32),
            pltpu.VMEM((2, rows, half), BF16),
            pltpu.VMEM((2, rows), I32),
            pltpu.VMEM((2, n_pos, rows), F32),
        ),
        in_specs=[vmem, vmem] + [any_spec] * 5,
        out_specs=(vmem,) * 10,
        scratch_shapes=[
            pltpu.VMEM((n_wire, 2 * fold), BF16),
            pltpu.VMEM((2, n_wire, 2 * fold), BF16),
            pltpu.VMEM((n_rows, width), BF16),
            pltpu.VMEM((n_rows, width), BF16),
            pltpu.VMEM((n_rows, 2 * ff), BF16),
            pltpu.VMEM((n_rows, ff), BF16),
            pltpu.VMEM((cr, half), BF16),
            pltpu.VMEM((cr, half), BF16),
            pltpu.VMEM((ng, cr, half), BF16),
            pltpu.VMEM((4, cr, wr), BF16),
            pltpu.VMEM((4, wr, cr), BF16),
            pltpu.VMEM((n_pos, 1, 128), F32),
            pltpu.VMEM((n_pos, 1, 128), F32),
            pltpu.VMEM((GS, 128), F32),
            pltpu.VMEM((ng, GS, 128), F32),
            pltpu.VMEM((n_pos, 1, 128), F32),
            pltpu.VMEM((16, width), F32),
            pltpu.VMEM((16, width), F32),
            pltpu.VMEM((ff, 128), F32),
            dma((2 * ng,)), dma((2 * ng,)), dma((ng,)), dma((ng,)),
            dma((2,)), dma((2 * ng,)), dma, dma((ng,)), dma, dma((ng,)),
            dma((ng,)), dma((ng,)), dma((ng,)), dma((ng,)),
            dma, dma, dma((5,)),
        ],
        compiler_params=pltpu.CompilerParams(
            collective_id=0, has_side_effects=True, vmem_limit_bytes=VMEM_K1
        ),
    )(experts.T, gates.T, tokens, cotangent, gate_w[0], up_w[0], down_w[0])
    outs = pl.pallas_call(
        flush,
        out_shape=(
            jax.ShapeDtypeStruct((rows, half), BF16),
            jax.ShapeDtypeStruct((2, rows), F32),
            jax.ShapeDtypeStruct((width, ff), BF16),
            jax.ShapeDtypeStruct((width, ff), BF16),
            jax.ShapeDtypeStruct((ff, width), BF16),
            jax.ShapeDtypeStruct((1, width), F32),
            jax.ShapeDtypeStruct((1, width), F32),
            jax.ShapeDtypeStruct((1, ff), F32),
        ),
        in_specs=[vmem] * 10,
        out_specs=(any_spec, vmem) + (any_spec,) * 6,
        scratch_shapes=[pltpu.VMEM((rows, half), BF16), dma((19,))],
        compiler_params=pltpu.CompilerParams(vmem_limit_bytes=VMEM_K2),
    )(*outs)
    gt, gg, ggw, guw, gdw, sqg, squ, sqd = outs
    return gt, gg.T, ggw[None], guw[None], gdw[None], sqg, squ, sqd


def solution(mesh):
    placed = (
        P("ep", None),
        P("ep", None),
        P("ep", None),
        P("ep", None),
        P("ep", None, "tp"),
        P("ep", None, "tp"),
        P("ep", "tp", None),
    )
    return jax.shard_map(
        body,
        mesh=mesh,
        in_specs=placed,
        out_specs=(
            P("ep", "tp"),
            P("ep", None),
            P("ep", None, "tp"),
            P("ep", None, "tp"),
            P("ep", "tp", None),
            P("ep", None),
            P("ep", None),
            P("ep", "tp"),
        ),
        check_vma=False,
    )
```
